32 devices in a mesh: sp: 16 (over z, y, core), tp: 2 (over x).
Axes of the slice: x: 2, y: 2, z: 4, core: 2. Of those that a mesh axis runs over, the one named last changes fastest.
Arguments:
- residual: bfloat16 [2048, 2048], P('sp', 'tp'), may hold values from -24 to 24
- queries: bfloat16 [2048, 2048], P('sp', 'tp'), may hold values from -16 to 16
- key_proj: bfloat16 [2048, 512], P(('sp', 'tp')), may hold values from -8 to 8
- value_proj: bfloat16 [2048, 512], P(('sp', 'tp')), may hold values from -6 to 6
- diff_lambda: float32 [8], replicated, may hold values from 0.3 to 0.8
- head_gain: float32 [256], replicated, may hold values from 0.1 to 1.9
- out_weight: bfloat16 [2048, 2048], P(None, 'tp'), may hold values from -0.125 to 0.125
- norm_gain: float32 [2048], P('tp'), may hold values from 0.1 to 1.9
- up_weight: bfloat16 [2048, 8192], P('sp', 'tp'), may hold values from -0.125 to 0.125
- down_weight: bfloat16 [8192, 2048], P('tp', 'sp'), may hold values from -0.0625 to 0.0625
Outputs:
- layer_out: bfloat16 [2048, 2048], P('sp', 'tp')
The draws below stay inside these ranges and needn't reach their ends.
All inputs are finite; a program needn't handle non-finite values.
Results may differ from the reference program's by a relative error of at most 0.012.
Values may be sent and summed in bfloat16 or wider, within the bound.
No kernel may reach another device: no remote copies, remote signals or barrier semaphores. Data moves between devices by JAX's collectives and lax.ppermute only.
A program may use at most 128 MiB of HBM per device.

```python
import jax
import jax.numpy as jnp
from jax import lax

D = 2048
HEADS = 8
KV_HEADS = 2
HEAD_DIM = 128
VALUE_DIM = 256
FF = 8192
TOK_DEV = 128
SEQ = 2048


def draw_residual(key, part):
    base = jax.random.fold_in(key, 11)
    first, second, third = jax.random.split(base, 3)
    noise = jax.random.truncated_normal(first, -3.0, 3.0, (SEQ, D), jnp.float32)
    column = jnp.arange(D, dtype=jnp.float32) / D
    rough = jnp.exp(jax.random.uniform(second, (1, D), jnp.float32, jnp.log(0.8), jnp.log(1.25)))
    col_scale = jnp.exp(jnp.log(0.3) + jnp.log(10.0) * column)[None, :] * rough
    row_scale = jnp.exp(jax.random.uniform(third, (SEQ, 1), jnp.float32, jnp.log(0.5), jnp.log(1.6)))
    return (noise * col_scale * row_scale).astype(jnp.bfloat16)


def drawn_pair(key):
    base = jax.random.fold_in(key, 23)
    streams = jax.random.split(base, 2)
    query_vals = 1.3 * jax.random.truncated_normal(streams[0], -6.0, 6.0, (SEQ, HEADS * 2 * HEAD_DIM), jnp.float32)
    key_vals = 1.3 * jax.random.truncated_normal(streams[1], -6.0, 6.0, (SEQ, KV_HEADS * 2 * HEAD_DIM), jnp.float32)
    return (query_vals, key_vals)


def draw_queries(key, part):
    return drawn_pair(key)[0].astype(jnp.bfloat16)


def draw_key_proj(key, part):
    return drawn_pair(key)[1].astype(jnp.bfloat16)


def levels(own_key, extent, cuts, least, largest):
    def one(position, shards_of):
        heights = jax.random.uniform(jax.random.fold_in(jax.random.fold_in(own_key, 6), position), (shards_of,), jnp.float32, least / len(cuts), largest / len(cuts))
        return jnp.repeat(jnp.exp(heights), extent[position] // shards_of).reshape((-1,) + (1,) * (len(extent) - position - 1))

    loudness = one(*cuts[0])
    for cut in cuts[1:]:
        loudness = loudness * one(*cut)
    return loudness


def normal_values(own_key, shape, deviation, most, shards=(), held_as=jnp.bfloat16):
    values = jax.random.normal(own_key, shape, jnp.float32) * deviation
    if len(shards) > 0:
        values = levels(own_key, shape, shards, -0.22, 0.18) * values
    return jnp.clip(values, min=-most, max=most).astype(held_as)


def setup_inputs(seed: int = 0) -> dict:
    key_list = jax.random.split(jax.random.key(seed), 11)
    residual = draw_residual(jax.random.fold_in(key_list[10], 71), 0)
    queries = draw_queries(jax.random.fold_in(key_list[10], 71), 0)
    key_proj = draw_key_proj(jax.random.fold_in(key_list[10], 71), 0)
    value_proj = normal_values(key_list[3], (SEQ, KV_HEADS * VALUE_DIM), 1.0, 6.0, ((0, 32),))
    diff_lambda = jnp.clip(jax.random.uniform(key_list[4], (HEADS,), jnp.float32, 0.3, 0.8), 0.3, 0.8)
    head_gain = jnp.clip(1.0 + 0.18 * jax.random.normal(key_list[5], (VALUE_DIM,), jnp.float32), 0.1, 1.9)
    out_weight = normal_values(key_list[6], (HEADS * VALUE_DIM, D), (HEADS * VALUE_DIM) ** -0.5, 0.125, ((1, 2),))
    norm_gain = jnp.clip(1.0 + 0.18 * jax.random.normal(key_list[7], (D,), jnp.float32), 0.1, 1.9)
    up_weight = normal_values(key_list[8], (D, FF), D ** -0.5, 0.125, ((0, 16), (1, 2)))
    down_weight = normal_values(key_list[9], (FF, D), FF ** -0.5, 0.0625, ((0, 2), (1, 16)))
    return dict(residual=residual, queries=queries, key_proj=key_proj, value_proj=value_proj, diff_lambda=diff_lambda, head_gain=head_gain, out_weight=out_weight, norm_gain=norm_gain, up_weight=up_weight, down_weight=down_weight)


epsilon = 1e-06

def reference(residual, queries, key_proj, value_proj, diff_lambda, head_gain, out_weight, norm_gain, up_weight, down_weight):
    per_group = HEADS // KV_HEADS
    seq_len = queries.shape[0]
    scaling = HEAD_DIM ** (-0.5)
    key_grid = key_proj.astype(jnp.float32).reshape(seq_len, KV_HEADS, 2, HEAD_DIM)
    value_grid = value_proj.astype(jnp.float32).reshape(seq_len, KV_HEADS, VALUE_DIM)
    lambdas = diff_lambda.reshape(KV_HEADS, per_group, 1, 1)
    blocks = queries.reshape(seq_len // TOK_DEV, TOK_DEV, KV_HEADS, per_group, 2, HEAD_DIM)

    def one_block(query_block):
        query_float = query_block.astype(jnp.float32)
        scores = jnp.einsum('qagcd,kacd->agcqk', query_float, key_grid) * scaling
        highest = lax.optimization_barrier(jnp.max(scores, axis=-1, keepdims=True))
        weights = jnp.exp(scores - highest)
        totals = lax.optimization_barrier(jnp.sum(weights, axis=-1))
        rounded = lax.optimization_barrier(weights.astype(jnp.bfloat16)).astype(jnp.float32)
        summed = jnp.einsum('agcqk,kae->agcqe', rounded, value_grid)
        per_map = summed / totals[..., None]
        difference = per_map[:, :, 0] - lambdas * per_map[:, :, 1]
        normed = difference * lax.rsqrt(lax.optimization_barrier(jnp.mean(difference * difference, axis=-1, keepdims=True)) + epsilon) * head_gain
        return normed.astype(jnp.bfloat16).reshape(HEADS, TOK_DEV, VALUE_DIM)
    outputs = lax.map(one_block, blocks)
    head_outputs = outputs.transpose(1, 0, 2, 3).reshape(HEADS, seq_len, VALUE_DIM)
    out_grid = out_weight.reshape(HEADS, VALUE_DIM, D)
    projected = jnp.einsum('hse,hed->sd', head_outputs.astype(jnp.float32), out_grid.astype(jnp.float32))
    after_mix = residual.astype(jnp.float32) + projected
    normed = (after_mix * lax.rsqrt(lax.optimization_barrier(jnp.mean(after_mix * after_mix, axis=1, keepdims=True)) + epsilon) * norm_gain).astype(jnp.bfloat16)
    hidden = jnp.dot(normed, up_weight, preferred_element_type=jnp.float32)
    activated = jnp.square(jax.nn.relu(hidden)).astype(jnp.bfloat16)
    mixed = jnp.dot(activated, down_weight, preferred_element_type=jnp.float32)
    return (after_mix + mixed).astype(jnp.bfloat16)
```

```python
import functools

import jax
import jax.numpy as jnp
from jax import lax
from jax.experimental import pallas as pl
from jax.experimental.pallas import tpu as pltpu
from jax.sharding import PartitionSpec as P

D = 2048
HEADS = 8
KV_HEADS = 2
HEAD_DIM = 128
VALUE_DIM = 256


epsilon = 1e-06


def attention_kernel(lambda_ref, q_ref, gain_ref, *refs):
    *kv_refs, out_ref = refs
    width = 2 * HEAD_DIM
    heads = q_ref.shape[1] // width
    rows = q_ref.shape[0]
    maps = []
    for c in range(2):
        q = jnp.concatenate(
            [q_ref[:, h * width + c * HEAD_DIM : h * width + (c + 1) * HEAD_DIM] for h in range(heads)],
            axis=0,
        )
        scores = [
            lax.dot_general(
                q,
                kv[:, c * HEAD_DIM : (c + 1) * HEAD_DIM],
                (((1,), (1,)), ((), ())),
                preferred_element_type=jnp.float32,
            )
            * (HEAD_DIM ** (-0.5))
            for kv in kv_refs
        ]
        highest = functools.reduce(jnp.maximum, [jnp.max(s, axis=1, keepdims=True) for s in scores])
        weights = [jnp.exp(s - highest) for s in scores]
        total = sum(jnp.sum(w, axis=1, keepdims=True) for w in weights)
        summed = sum(
            jnp.dot(w.astype(jnp.bfloat16), kv[:, width:], preferred_element_type=jnp.float32)
            for w, kv in zip(weights, kv_refs)
        )
        maps.append(summed / total)
    for h in range(heads):
        here = slice(h * rows, (h + 1) * rows)
        difference = maps[0][here] - lambda_ref[h] * maps[1][here]
        scaled = (
            difference
            * lax.rsqrt(jnp.mean(difference * difference, axis=1, keepdims=True) + epsilon)
            * gain_ref[...]
        )
        out_ref[:, h * VALUE_DIM : (h + 1) * VALUE_DIM] = scaled.astype(jnp.bfloat16)


def attention(queries, kv_parts, lambdas, gain):
    rows = queries.shape[0]
    heads = lambdas.shape[0]
    vmem = pl.BlockSpec(memory_space=pltpu.VMEM)
    return pl.pallas_call(
        attention_kernel,
        out_shape=jax.ShapeDtypeStruct((rows, heads * VALUE_DIM), jnp.bfloat16),
        in_specs=[pl.BlockSpec(memory_space=pltpu.SMEM), vmem, vmem] + [vmem] * len(kv_parts),
        out_specs=vmem,
        compiler_params=pltpu.CompilerParams(vmem_limit_bytes=48 * 1024 * 1024),
    )(lambdas, queries, gain[None, :], *kv_parts)


def on_device(
    residual,
    queries,
    key_proj,
    value_proj,
    diff_lambda,
    head_gain,
    out_weight,
    norm_gain,
    up_weight,
    down_weight,
):
    sp_size = lax.axis_size("sp")
    tp_size = lax.axis_size("tp")
    outer = 1 << (sp_size.bit_length() // 2)
    if outer * outer > sp_size:
        outer //= 2
    inner = sp_size // outer
    sp_at = lax.axis_index("sp")
    tp_at = lax.axis_index("tp")
    outer_at = sp_at // inner
    inner_at = sp_at % inner

    def along_outer(value, shift):
        return lax.ppermute(
            value, "sp", [(s, (s + shift * inner) % sp_size) for s in range(sp_size)]
        )

    def along_inner(value, flip):
        return lax.ppermute(value, "sp", [(s, s ^ flip) for s in range(sp_size)])

    def along_tp(value, shift):
        return lax.ppermute(value, "tp", [(t, (t + shift) % tp_size) for t in range(tp_size)])

    flips = [1 << b for b in reversed(range(inner.bit_length() - 1))]

    group_width = 2 * HEAD_DIM
    both = jnp.stack(
        [
            jnp.concatenate(
                [
                    key_proj[:, a * group_width : (a + 1) * group_width],
                    value_proj[:, a * VALUE_DIM : (a + 1) * VALUE_DIM],
                ],
                axis=1,
            )
            for a in range(KV_HEADS)
        ]
    )

    def of_group(t):
        return lax.dynamic_index_in_dim(both, (t % tp_size) * KV_HEADS // tp_size, 0, keepdims=False)

    kv_own = jnp.concatenate(
        [of_group(tp_at)] + [along_tp(of_group(tp_at + k), k) for k in range(1, tp_size)], axis=0
    )
    kv_outer = [kv_own] + [along_outer(kv_own, d) for d in range(1, outer)]
    kv_outer, up_weight, down_weight = lax.optimization_barrier(
        (kv_outer, up_weight, down_weight)
    )
    kv_pieces = kv_outer
    for flip in flips[:-1]:
        kv_pieces = kv_pieces + [along_inner(piece, flip) for piece in kv_pieces]
    kv_chip = jnp.concatenate(kv_pieces, axis=0)
    kv_parts = [kv_chip] + [along_inner(kv_chip, flip) for flip in flips[-1:]]

    hidden_here = up_weight.shape[1] // outer
    up_rows = up_weight.shape[0]
    down_cols = down_weight.shape[1]
    per_tp = sp_size // tp_size

    def place(source):
        return (tp_at - source // per_tp) % tp_size * per_tp + source % per_tp

    def gather_weight(weight, axis):
        pieces = []
        for d in range(outer):
            cut = lax.dynamic_slice_in_dim(
                weight, (outer_at + d) % outer * hidden_here, hidden_here, axis
            )
            got = along_outer(cut, d) if d else cut
            pieces.append(((outer_at - d) % outer, 0, got))
        for flip in flips:
            pieces = pieces + [(z, e ^ flip, along_inner(p, flip)) for z, e, p in pieces]
        return [(place(z * inner + (inner_at ^ e)), p) for z, e, p in pieces]

    up_full = jnp.zeros((up_rows * sp_size, hidden_here), up_weight.dtype)
    for at, piece in gather_weight(up_weight, 1):
        up_full = lax.dynamic_update_slice(up_full, piece, (at * up_rows, 0))
    down_full = jnp.zeros((hidden_here, down_cols * sp_size), down_weight.dtype)
    for at, piece in gather_weight(down_weight, 0):
        down_full = lax.dynamic_update_slice(down_full, piece, (0, at * down_cols))

    heads_here = HEADS // tp_size
    lambdas = lax.dynamic_slice_in_dim(diff_lambda, tp_at * heads_here, heads_here)
    own_heads = attention(queries, kv_parts, lambdas, head_gain)
    head_width = own_heads.shape[1]
    head_outputs = jnp.zeros((own_heads.shape[0], head_width * tp_size), own_heads.dtype)
    for k in range(tp_size):
        got = along_tp(own_heads, k) if k else own_heads
        head_outputs = lax.dynamic_update_slice(
            head_outputs, got, (0, (tp_at - k) % tp_size * head_width)
        )
    after_mix = residual.astype(jnp.float32) + jnp.dot(
        head_outputs, out_weight, preferred_element_type=jnp.float32
    )
    own_squares = jnp.sum(after_mix * after_mix, axis=1, keepdims=True)
    gained = (after_mix * norm_gain).astype(jnp.bfloat16)

    blocks = [gained] + [along_outer(gained, d) for d in range(1, outer)]
    squares = own_squares
    for k in range(1, tp_size):
        squares = squares + along_tp(own_squares, k)
    width = gained.shape[1]
    mixed = jnp.zeros(after_mix.shape, jnp.float32)
    for d, block in enumerate(blocks):
        rows = jnp.concatenate(
            [block] + [along_tp(block, k) for k in range(1, tp_size)], axis=1
        )
        hidden = jnp.dot(rows, up_full, preferred_element_type=jnp.float32)
        activated = jnp.square(jax.nn.relu(hidden)).astype(jnp.bfloat16)
        partial_value = jnp.dot(activated, down_full, preferred_element_type=jnp.float32)
        total = partial_value[:, :width]
        for k in range(1, tp_size):
            away = partial_value[:, k * width : (k + 1) * width].astype(jnp.bfloat16)
            total = total + along_tp(away, -k).astype(jnp.float32)
        if d:
            total = along_outer(total.astype(jnp.bfloat16), -d).astype(jnp.float32)
        mixed = mixed + total
    factor = 1.0 / (squares / D + epsilon)
    return (after_mix + factor * mixed).astype(jnp.bfloat16)


def solution(mesh):
    return jax.shard_map(
        on_device,
        mesh=mesh,
        in_specs=(
            P("sp", "tp"),
            P("sp", "tp"),
            P(("sp", "tp"), None),
            P(("sp", "tp"), None),
            P(),
            P(),
            P(None, "tp"),
            P("tp"),
            P("sp", "tp"),
            P("tp", "sp"),
        ),
        out_specs=P("sp", "tp"),
        check_vma=False,
    )
```
